32 devices in a mesh: ep: 8 (over z, x), tp: 4 (over y, core).
Axes of the slice: x: 2, y: 2, z: 4, core: 2. Of those that a mesh axis runs over, the one named last changes fastest.
Arguments:
- tokens: bfloat16 [2048, 2048], P('ep'), may hold values from -6 to 6
- norm_gain: float32 [2048], replicated, may hold values from 0.1 to 1.9
- expert_ids: int32 [2048, 4], P('ep'), may hold values from 0 to 7, all different within a row; in each aligned block of 256 rows (0 to 255, 256 to 511, ...) at most 256 rows name the same one
- route_weights: float32 [2048, 4], P('ep'), may hold values from 0.05 to 1
- gate_weight: bfloat16 [8, 2048, 2048], P('ep', None, 'tp'), as said below
- up_weight: bfloat16 [8, 2048, 2048], P('ep', None, 'tp'), as said below
- down_weight: bfloat16 [8, 2048, 2048], P('ep', 'tp'), may hold values from -0.125 to 0.125
Outputs:
- mixed: bfloat16 [2048, 2048], P('ep', 'tp')
The draws below stay inside these ranges and needn't reach their ends.
Inputs may be any that keep to these rules, and one draw needn't show every extreme that they name: `expert_ids`: each row names 4 different experts. In the rows of one device no expert is named by more than 256 rows, and in every draw some expert is named by exactly 256 rows of some device. `gate_weight`: independent entries of mean zero, drawn for each expert separately. `up_weight`: independent entries of mean zero, drawn for each expert separately.
All inputs are finite; a program needn't handle non-finite values.
Results may differ from the reference program's by a relative error of at most 0.014.
Values may be sent and summed in bfloat16 or wider, within the bound.
A program may use at most 128 MiB of HBM per device.

```python
import math
import jax
import jax.numpy as jnp
import numpy as np
from jax import lax

D = 2048
FF = 2048
TOP = 4
TOK_DEV = 256
EXPERTS = 8
CAP = 256
TOKENS = 2048
N_TP = 4


def draw_gate_weight(key, part):
    factor = 1.0
    values = jax.random.normal(jax.random.fold_in(key, 11), (EXPERTS, D, FF), jnp.float32)
    return (values * (factor / D ** 0.5)).astype(jnp.bfloat16)


def draw_up_weight(key, part):
    factor = 1.0
    values = jax.random.normal(jax.random.fold_in(key, 23), (EXPERTS, D, FF), jnp.float32)
    return (values * (factor / D ** 0.5)).astype(jnp.bfloat16)


def levels(stream_key, shape, split, smallest, largest):
    gain, own = 1.0, jax.random.fold_in(stream_key, 6)
    for dim, blocks in split:
        draws = jnp.exp(jax.random.uniform(jax.random.fold_in(own, dim), (blocks,), jnp.float32, smallest / len(split), largest / len(split)))
        gain = gain * jnp.repeat(draws, shape[dim] // blocks).reshape([-1 if axis == dim else 1 for axis in range(len(shape))])
    return gain


def deal_out(own_key, own, number, rows, count, top, most, lean):
    sequence = jax.random.permutation(own_key, count)
    heavy_load, ordinary = portions_of(count, rows * top, most, lean, True), portions_of(count, rows * top, most, lean, False)
    places = jnp.arange(count)

    def named(lengths, rotation):
        used = int((lengths > 0).sum())
        fixed = max(1, used // 4)
        moved = fixed + (places - fixed + rotation * (used - fixed)) % max(1, count - fixed)
        return jnp.zeros((count,), jnp.int32).at[sequence[jnp.where(places < fixed, places, moved)]].set(jnp.asarray(lengths, jnp.int32))

    lengths = jnp.where(number % 4 == 0, named(heavy_load, number // 4), named(ordinary, number - number // 4 - 1))
    mixed = jax.random.permutation(jax.random.fold_in(own, 3), count)
    source_of, sink = mixed[0:count // 2 * 2:2], mixed[1:count // 2 * 2:2]
    slack = jnp.minimum(lengths[source_of] - 1, most - lengths[sink]) // 2
    slack = jnp.where((source_of == sequence[0]) | (sink == sequence[0]) | (lengths[sink] == 0), 0, jnp.maximum(slack, 0))
    moved = jax.random.randint(jax.random.fold_in(own, 4), (count // 2,), 0, 1 << 20) % (slack + 1)
    lengths = lengths.at[source_of].add(-moved).at[sink].add(moved)
    labels = jnp.searchsorted(jnp.cumsum(lengths), jnp.arange(rows * top), side="right").astype(jnp.int32)
    listing = labels.reshape(top, rows).T
    listing = listing[jax.random.permutation(jax.random.fold_in(own, 1), rows)]
    rotation = jax.random.randint(jax.random.fold_in(own, 2), (rows, 1), 0, top)
    return jnp.take_along_axis(listing, (jnp.arange(top)[None, :] + rotation) % top, axis=1)


def portions_of(number_of, total, reach, slope, full):
    portions = [(1 << 20) // math.isqrt(standing ** slope) + 1 for standing in range(1, number_of + 1)]
    largest = reach if full else min(reach, max(-(-total // number_of), total * portions[0] // sum(portions)))
    least = 1 if total - largest >= number_of - 1 else 0
    holding, rest = [largest] + [least] * (number_of - 1), total - largest - least * (number_of - 1)
    while rest > 0:
        movable = [i for i in range(1, number_of) if holding[i] < largest] or [i for i in range(1, number_of) if holding[i] < reach]
        pool, remaining = sum([portions[i] for i in movable]), rest
        for i in movable:
            extra = min(reach - holding[i], max(1, remaining * portions[i] // pool), rest)
            holding[i] = holding[i] + extra
            rest = rest - extra
    return np.array(holding)


def scatter_about(stream_key, dims, scale, reach, shards=(), held_as=jnp.bfloat16):
    values = scale * jax.random.normal(stream_key, dims, jnp.float32)
    if shards:
        values = values * levels(stream_key, dims, shards, -0.22, 0.18)
    return jnp.clip(values, -reach, reach).astype(held_as)


def setup_inputs(seed: int = 0) -> dict:
    key_of = jax.random.split(jax.random.key(seed), 8)
    tokens = scatter_about(key_of[0], (TOKENS, D), 1.0, 6.0, ((0, 8),))
    norm_gain = jnp.clip(1.0 + 0.18 * jax.random.normal(key_of[1], (D,), jnp.float32), 0.1, 1.9)
    expert_ids_keys = jax.random.split(jax.random.fold_in(key_of[2], 1), TOKENS // TOK_DEV)
    expert_ids_turns = jax.random.permutation(jax.random.fold_in(key_of[2], 3), TOKENS // TOK_DEV)
    expert_ids = jax.vmap(lambda own, number: deal_out(jax.random.fold_in(key_of[2], 2), own, number, TOK_DEV, EXPERTS, TOP, CAP, 2))(expert_ids_keys, expert_ids_turns).reshape((TOKENS, TOP))
    route_weights = jnp.clip(0.05 + 0.95 * jax.random.uniform(key_of[3], (TOKENS, TOP), jnp.float32) ** levels(key_of[3], (TOKENS, TOP), ((0, 8),), -0.2, 0.2), 0.05, 1.0)
    gate_weight = draw_gate_weight(jax.random.fold_in(key_of[7], 71), 0)
    up_weight = draw_up_weight(jax.random.fold_in(key_of[7], 71), 0)
    down_weight = scatter_about(key_of[6], (EXPERTS, FF, D), FF ** -0.5, 0.125, ((0, 8), (1, 4)))
    return dict(tokens=tokens, norm_gain=norm_gain, expert_ids=expert_ids, route_weights=route_weights, gate_weight=gate_weight, up_weight=up_weight, down_weight=down_weight)


def reference(tokens, norm_gain, expert_ids, route_weights, gate_weight, up_weight, down_weight):
    values = tokens.astype(jnp.float32)
    scale = lax.rsqrt(lax.optimization_barrier(jnp.mean(values * values, axis=1, keepdims=True)) + 1e-06)
    normed = (values * scale * norm_gain[None, :]).astype(jnp.bfloat16)
    blocks = TOKENS // TOK_DEV
    pairs_dev = TOK_DEV * TOP
    flat = expert_ids.reshape(blocks, pairs_dev)
    onehot = (flat[:, :, None] == jnp.arange(EXPERTS, dtype=jnp.int32)[None, None, :]).astype(jnp.int32)
    before = jnp.cumsum(onehot, axis=1) - onehot
    slot = lax.optimization_barrier(jnp.sum(before * onehot, axis=2))
    source = jnp.arange(blocks, dtype=jnp.int32)[:, None]
    position = (slot + source * CAP).reshape(-1).astype(jnp.int32)
    pair_tok = (source * TOK_DEV + jnp.arange(pairs_dev, dtype=jnp.int32)[None, :] // TOP).reshape(-1).astype(jnp.int32)
    expert_flat = flat.reshape(-1).astype(jnp.int32)
    rows = blocks * CAP
    tok_table = jnp.zeros((EXPERTS, rows), jnp.int32).at[expert_flat, position].set(pair_tok)
    weight_table = jnp.zeros((EXPERTS, rows), jnp.float32).at[expert_flat, position].set(route_weights.reshape(-1))

    def one_expert(total, index):
        chosen = normed[tok_table[index]]
        gate = jnp.dot(chosen, gate_weight[index], preferred_element_type=jnp.float32)
        upper = jnp.dot(chosen, up_weight[index], preferred_element_type=jnp.float32)
        gate = jnp.minimum(gate, 7.0)
        upper = jnp.clip(upper, -7.0, 7.0)
        hidden = ((upper + 1.0) * (gate * jax.nn.sigmoid(1.702 * gate))).astype(jnp.bfloat16)
        blocked = hidden.reshape(rows, N_TP, FF // N_TP).astype(jnp.float32)
        down_blocks = down_weight[index].reshape(N_TP, FF // N_TP, D).astype(jnp.float32)
        partial_value = jnp.einsum('rpf,pfd->rpd', blocked, down_blocks).astype(jnp.bfloat16)
        expert_out = lax.optimization_barrier(jnp.sum(partial_value.astype(jnp.float32), axis=1)).astype(jnp.bfloat16)
        total = total.at[tok_table[index]].add(weight_table[index][:, None] * expert_out.astype(jnp.float32))
        return (total, None)
    start = jnp.zeros((TOKENS, D), jnp.float32)
    total, unused = lax.scan(one_expert, start, jnp.arange(EXPERTS, dtype=jnp.int32))
    return total.astype(jnp.bfloat16)
```

```python
import functools

import jax
import jax.numpy as jnp
from jax import lax
from jax.experimental import pallas as pl
from jax.experimental.pallas import tpu as pltpu
from jax.sharding import PartitionSpec as P


MESH = pl.DeviceIdType.MESH


def normalise(tokens, norm_gain):
    values = tokens.astype(jnp.float32)
    scale = lax.rsqrt(jnp.mean(values * values, axis=1, keepdims=True) + 1e-06)
    return (values * scale * norm_gain[None, :]).astype(jnp.bfloat16)


def activate(gate, upper):
    gate = jnp.minimum(gate, 7.0)
    upper = jnp.clip(upper, -7.0, 7.0)
    return (upper + 1.0) * (gate * jax.nn.sigmoid(1.702 * gate))


def routed(tokens, norm_gain, expert_ids, route_weights, gate_weight, up_weight, down_weight):
    tok_dev, width = tokens.shape
    top = expert_ids.shape[1]
    n_ep = lax.axis_size("ep")
    n_tp = lax.axis_size("tp")
    exp_dev = gate_weight.shape[0]
    experts = exp_dev * n_ep
    capacity = 2 * tok_dev * top // experts
    quarter = width // n_tp
    normed = normalise(tokens, norm_gain)
    flat = expert_ids.reshape(-1)
    count = flat.shape[0]
    onehot = (flat[:, None] == jnp.arange(experts, dtype=jnp.int32)[None, :]).astype(jnp.int32)
    before = jnp.cumsum(onehot, axis=0) - onehot
    slot = jnp.sum(before * onehot, axis=1)
    position = flat * capacity + slot
    source_tok = jnp.arange(count, dtype=jnp.int32) // top
    buffer_tok = jnp.zeros((experts * capacity,), jnp.int32).at[position].set(source_tok)
    buffer_live = jnp.zeros((experts * capacity,), jnp.int32).at[position].set(1)
    columns = lax.dynamic_slice_in_dim(normed, lax.axis_index("tp") * quarter, quarter, 1)
    outgoing = jnp.where(buffer_live[:, None] > 0, columns[buffer_tok], jnp.zeros((), jnp.bfloat16))
    outgoing = outgoing.reshape(n_ep, exp_dev, capacity, quarter)
    received = lax.all_gather(
        lax.all_to_all(outgoing, "ep", split_axis=0, concat_axis=0, tiled=True),
        "tp",
        axis=3,
        tiled=True,
    )
    gate = jnp.einsum("sxcd,xdf->sxcf", received, gate_weight, preferred_element_type=jnp.float32)
    upper = jnp.einsum("sxcd,xdf->sxcf", received, up_weight, preferred_element_type=jnp.float32)
    hidden = activate(gate, upper).astype(jnp.bfloat16)
    partial_value = jnp.einsum(
        "sxcf,xfd->sxcd", hidden, down_weight, preferred_element_type=jnp.float32
    )
    rounded = partial_value.astype(jnp.bfloat16)
    summed = lax.psum_scatter(rounded, "tp", scatter_dimension=3, tiled=True)
    returned = lax.all_to_all(summed, "ep", split_axis=0, concat_axis=0, tiled=True)
    returned = returned.reshape(experts * capacity, quarter)
    picked = returned[position].reshape(tok_dev, top, quarter)
    mixed = jnp.sum(route_weights[:, :, None] * picked.astype(jnp.float32), axis=1)
    return mixed.astype(jnp.bfloat16)


XZ = (False, False, True, True)
SPECIAL = 8
END = (
    ("F", 0, -1), ("N", 0, -1), ("P", 0, 1, 3), ("P", 1, 0, 0), ("P", 0, 1, 2),
    ("P", 1, 0, 1), ("Y", 0, 1, 3), ("Y", 1, 0, 0), ("P", 0, 1, 1), ("P", 1, 0, 2),
    ("Y", 0, 1, 2), ("Y", 1, 0, 1), ("P", 0, 1, 0), ("P", 1, 0, 3), ("Y", 0, 1, 1),
    ("Y", 1, 0, 2), ("P", 1, 1, 0), ("P", 2, 0, 0), ("Y", 0, 1, 0), ("Y", 1, 0, 3),
    ("F", 0, -2), ("P", 1, 1, 3), ("Y", 1, 1, 0), ("P", 1, 1, 1), ("N", 0, -2),
    ("P", 1, 1, 2), ("F", 1, 0), ("A", 0, 0), ("A", 0, 2), ("Y", 1, 1, 3),
    ("P", 2, 1, 0), ("A", 0, 1), ("N", 1, 0), ("Y", 1, 1, 2), ("P", 2, 0, 1),
    ("F", 1, 3), ("A", 1, 0), ("P", 2, 0, 2), ("N", 1, 3), ("Bb", 0, 0),
    ("Y", 2, 0, 0), ("Y", 1, 1, 1), ("W", 0, 0), ("A", 1, 3), ("Ba", 0, 2),
    ("Bb", 0, 2), ("Ba", 0, 0), ("P", 2, 0, 3), ("F", 1, 2), ("Y", 2, 1, 0),
    ("N", 1, 2), ("Bb", 0, 1), ("Ba", 0, 1), ("F", 1, 1), ("P", 2, 1, 1),
    ("Y", 2, 0, 2), ("P", 2, 1, 3), ("N", 1, 1), ("P", 3, 0, 0), ("F", 2, 0),
    ("C", 0, 0), ("A", 1, 1), ("C", 0, 2), ("Y", 2, 0, 3), ("N", 2, 0),
    ("P", 2, 1, 2), ("C", 0, 1), ("Y", 2, 1, 1), ("A", 1, 2), ("A", 2, 0),
    ("Y", 2, 0, 1), ("Y", 2, 1, 3), ("W", 1, 0), ("P", 3, 0, 1), ("P", 3, 1, 0),
    ("Y", 3, 0, 0), ("F", 2, 1), ("Y", 2, 1, 2), ("N", 2, 1), ("P", 3, 0, 2),
    ("Bb", 2, 0), ("F", 2, 2), ("A", 2, 1), ("N", 2, 2), ("P", 3, 1, 1),
    ("P", 3, 0, 3), ("Y", 3, 1, 0), ("Ba", 2, 0), ("Y", 3, 0, 2), ("Y", 3, 0, 1),
    ("F", 2, 3), ("A", 2, 2), ("N", 2, 3), ("P", 3, 1, 3), ("Bb", 2, 1),
    ("F", 3, 0), ("A", 2, 3), ("Y", 3, 1, 1), ("P", 3, 1, 2), ("C", 2, 0),
    ("Ba", 2, 1), ("N", 3, 0), ("Bb", 2, 2), ("Y", 3, 0, 3), ("W", 2, 0),
    ("A", 3, 0), ("Y", 3, 1, 3), ("Ba", 2, 2), ("A", 0, 3), ("F", 3, 1),
    ("Bb", 2, 3), ("C", 2, 1), ("N", 3, 1), ("Ba", 2, 3), ("F", 3, 3),
    ("A", 3, 1), ("Bb", 3, 0), ("C", 2, 2), ("N", 3, 3), ("Y", 3, 1, 2),
    ("Ba", 3, 0), ("W", 1, 1), ("Bb", 0, 3), ("A", 3, 3), ("Ba", 0, 3),
    ("F", 3, 2), ("C", 2, 3), ("N", 3, 2), ("Ba", 3, 1), ("Bb", 3, 1),
    ("W", 2, 1), ("C", 3, 0), ("A", 3, 2), ("Bb", 3, 3), ("W", 3, 0),
    ("C", 0, 3), ("Ba", 3, 3), ("W", 0, 1), ("C", 3, 1), ("Ba", 3, 2),
    ("Bb", 3, 2), ("C", 3, 3), ("S", 0), ("C", 3, 2), ("W", 3, 1),
    ("S", 1), ("S", 3), ("S", 2),
)
MIDDLE = (
    ("F", 0, -1), ("N", 0, -1), ("P", 2, 0, 0), ("P", 0, 1, 3), ("P", 1, 0, 0),
    ("P", 0, 1, 2), ("P", 2, 0, 1), ("P", 1, 0, 1), ("Y", 2, 0, 0), ("Y", 0, 1, 3),
    ("Y", 1, 0, 0), ("P", 0, 1, 1), ("P", 2, 0, 2), ("P", 1, 0, 2), ("Y", 0, 1, 2),
    ("Y", 2, 0, 1), ("Y", 1, 0, 1), ("P", 0, 1, 0), ("P", 1, 0, 3), ("P", 2, 0, 3),
    ("Y", 0, 1, 1), ("Y", 2, 0, 2), ("Y", 1, 0, 2), ("P", 1, 1, 3), ("P", 2, 1, 0),
    ("P", 2, 1, 3), ("Y", 0, 1, 0), ("Y", 1, 0, 3), ("F", 0, -2), ("P", 1, 1, 2),
    ("P", 3, 0, 0), ("P", 1, 1, 0), ("Y", 1, 1, 3), ("N", 0, -2), ("Y", 2, 1, 3),
    ("P", 2, 1, 2), ("F", 1, 3), ("Y", 2, 1, 0), ("P", 2, 1, 1), ("N", 1, 3),
    ("P", 3, 0, 1), ("Y", 3, 0, 0), ("P", 1, 1, 1), ("Y", 2, 0, 3), ("Y", 1, 1, 2),
    ("F", 2, 0), ("A", 1, 3), ("Y", 1, 1, 0), ("Y", 2, 1, 2), ("N", 2, 0),
    ("P", 3, 0, 2), ("Y", 3, 0, 1), ("Y", 2, 1, 1), ("P", 3, 1, 0), ("F", 2, 3),
    ("Y", 1, 1, 1), ("A", 2, 0), ("P", 3, 1, 1), ("P", 3, 0, 3), ("N", 2, 3),
    ("F", 2, 1), ("Bb", 1, 3), ("Y", 3, 0, 2), ("P", 3, 1, 3), ("A", 2, 3),
    ("Ba", 1, 3), ("Y", 3, 1, 0), ("N", 2, 1), ("Ba", 2, 0), ("Bb", 2, 0),
    ("F", 3, 0), ("P", 3, 1, 2), ("Y", 3, 1, 1), ("A", 2, 1), ("Y", 3, 0, 3),
    ("N", 3, 0), ("F", 1, 1), ("Y", 3, 1, 3), ("C", 1, 3), ("A", 3, 0),
    ("Bb", 2, 3), ("N", 1, 1), ("Bb", 2, 1), ("Ba", 2, 3), ("F", 3, 3),
    ("C", 2, 0), ("A", 1, 1), ("Y", 3, 1, 2), ("N", 3, 3), ("Bb", 3, 0),
    ("F", 3, 2), ("Ba", 3, 0), ("A", 3, 3), ("N", 3, 2), ("Bb", 1, 1),
    ("Ba", 2, 1), ("F", 1, 0), ("A", 3, 2), ("Ba", 1, 1), ("N", 1, 0),
    ("C", 3, 0), ("C", 2, 3), ("W", 0, 0), ("A", 1, 0), ("Bb", 3, 3),
    ("C", 2, 1), ("A", 0, 1), ("Ba", 3, 3), ("F", 3, 1), ("N", 3, 1),
    ("Ba", 3, 2), ("C", 1, 1), ("Bb", 3, 2), ("W", 3, 0), ("A", 3, 1),
    ("Ba", 1, 0), ("Bb", 1, 0), ("F", 2, 2), ("Bb", 0, 1), ("N", 2, 2),
    ("A", 0, 2), ("Ba", 0, 1), ("A", 2, 2), ("C", 3, 2), ("W", 2, 0),
    ("C", 3, 3), ("F", 1, 2), ("C", 1, 0), ("Bb", 3, 1), ("N", 1, 2),
    ("Ba", 3, 1), ("Bb", 0, 2), ("W", 1, 0), ("Ba", 0, 2), ("A", 1, 2),
    ("C", 0, 1), ("S", 1), ("A", 0, 3), ("A", 0, 0), ("Bb", 2, 2),
    ("Ba", 2, 2), ("C", 3, 1), ("W", 3, 1), ("C", 0, 2), ("Bb", 1, 2),
    ("Ba", 1, 2), ("Bb", 0, 3), ("Ba", 0, 3), ("Bb", 0, 0), ("Ba", 0, 0),
    ("C", 2, 2), ("W", 2, 1), ("C", 1, 2), ("W", 1, 1), ("C", 0, 3),
    ("C", 0, 0), ("S", 0), ("S", 3), ("W", 0, 1), ("S", 2),
)


def kernel(
    n_ep, tokens_ref, gain_ref, route_ref, gate_hbm, up_hbm, down_hbm, out_ref,
    gath, gtab, route_buf, gate_w, up_w, down_w, hidden, part, dbuf, ya, xa, xb, yb, own, zin, raw,
    w_sem, st, rt, rp, sz, sx, sy, ry, sg, rg,
    s_d, r_d, s_ya, r_ya, s_xb, r_xb, s_xa, r_xa, s_yb, r_yb, s_z, r_z, s_raw, r_raw,
):
    ep, tp = lax.axis_index("ep"), lax.axis_index("tp")
    z, x, y, c = ep // 2, ep % 2, tp // 2, tp % 2
    nz = n_ep // 2
    width = tokens_ref.shape[1]
    quarter = width // 4
    eighth = quarter // 2
    side = width // 2
    special = width // SPECIAL
    primary = side - special
    pieces = len(XZ)
    rows = tokens_ref.shape[0] // pieces
    mine, other = ep, 2 * z + 1 - x
    toward = jnp.where(z < nz // 2, 1, -1)
    at_end = (z == 0) | (z == nz - 1)
    inward = {"ep": lax.rem(ep + 2 * toward + n_ep, n_ep), "tp": tp}
    outward = {"ep": lax.rem(ep - 2 * toward + n_ep, n_ep), "tp": tp}
    xdev = {"ep": other, "tp": tp}
    ydev = {"ep": ep, "tp": 2 * (1 - y) + c}
    ddev = {"ep": ep, "tp": 2 * y + 1 - c}

    weight_copies = [
        pltpu.make_async_copy(gate_hbm.at[0], gate_w, w_sem.at[0]),
        pltpu.make_async_copy(up_hbm.at[0], up_w, w_sem.at[1]),
        pltpu.make_async_copy(down_hbm.at[0], down_w, w_sem.at[2]),
    ]
    for item in weight_copies:
        item.start()

    barrier = pltpu.get_barrier_semaphore()

    def greet(device):
        pl.semaphore_signal(barrier, inc=1, device_id=device, device_id_type=MESH)

    def peer(k):
        return {"ep": lax.rem(ep + k, n_ep), "tp": tp}

    for device in (ydev, ddev):
        greet(device)
    for k in range(1, n_ep):
        greet(peer(k))

    tile = 32

    def norm_step(i, carry):
        at = pl.ds(pl.multiple_of(i * tile, tile), tile)
        values = tokens_ref[at, :].astype(jnp.float32)
        scale = lax.rsqrt(jnp.mean(values * values, axis=1, keepdims=True) + 1e-06)
        gath[ep, at, :] = (values * scale * gain_ref[...]).astype(jnp.bfloat16)
        return carry

    lax.fori_loop(0, tokens_ref.shape[0] // tile, norm_step, 0)
    gtab[ep] = route_ref[ep]
    pl.semaphore_wait(barrier, n_ep + 1)

    def span(start, size):
        return pl.ds(pl.multiple_of(start, 128), size)

    def send(src, dst, send_sem, recv_sem, device):
        return pltpu.make_async_remote_copy(
            src_ref=src, dst_ref=dst, send_sem=send_sem, recv_sem=recv_sem,
            device_id=device, device_id_type=MESH,
        )

    def band(h):
        start = h * rows
        return pl.ds(start if isinstance(start, int) else pl.multiple_of(start, 16), rows)

    def move(block, h, start, size, device, send_sem, recv_sem):
        ref = gath.at[block, band(h), span(start, size)]
        return send(ref, ref, send_sem, recv_sem, device)

    def go_main(block, h, device, send_sem):
        return move(block, h, c * side + y * special, primary, device, send_sem, rp.at[block, h])

    def go_z(block, h, way):
        return go_main(block, h, inward if way == 0 else outward, sz.at[way, block, h])

    def go_x(block, h):
        return go_main(block, h, xdev, sx.at[block, h])

    def go_y(block, h, yy):
        start = c * side + yy * primary
        return move(block, h, start, special, ydev, sy.at[block, h], ry.at[block, h])

    def go_d(block, h, kind, cc):
        start = cc * side + (y * special if kind == 0 else (1 - y) * primary)
        size = primary if kind == 0 else special
        return move(block, h, start, size, ddev, sg.at[kind, block, h], rg.at[kind, block, h])

    def table(k):
        target = lax.rem(ep + k, n_ep)
        return send(route_ref.at[target], gtab.at[ep], st.at[k], rt.at[ep], peer(k))

    def table_wait(block):
        return send(route_ref.at[ep], gtab.at[block], st.at[0], rt.at[block], xdev)

    for k in range(1, n_ep):
        table(k).start()
    slow_first = [h for h in range(pieces) if not XZ[h]] + [h for h in range(pieces) if XZ[h]]
    for h in slow_first[::-1]:
        go_x(mine, h).start()
    for h in slow_first:
        go_z(mine, h, 0).start()

        @pl.when(~at_end)
        def _():
            go_z(mine, h, 1).start()

    def got(block, h):
        go_x(block, h).wait_recv()

    def spread(block, h):
        go_y(block, h, y).start()
        go_d(block, h, 0, c).start()

    def on_y(block, h):
        go_y(block, h, 1 - y).wait_recv()
        go_d(block, h, 1, c).start()

    def ready(block, h):
        for kind in (0, 1):
            go_d(block, h, kind, 1 - c).wait_recv()

    def d_copy(b, h, yq, cc):
        return send(
            part.at[b, band(h), span((2 * yq + cc) * quarter, quarter)],
            dbuf.at[b, band(h), span(yq * quarter, quarter)],
            s_d.at[b, h, yq], r_d.at[b, h, yq], ddev,
        )

    def ya_copy(r, h):
        return send(
            dbuf.at[pl.ds(2 * r, 2), band(h), span((1 - y) * quarter, eighth)],
            ya.at[pl.ds(2 * r, 2), band(h)], s_ya.at[r, h], r_ya.at[r, h], ydev,
        )

    def xb_copy(r, h, yq):
        return send(
            dbuf.at[2 * r + 1 - x, band(h), span(yq * quarter + eighth, eighth)],
            xb.at[r, band(h), span(yq * eighth, eighth)],
            s_xb.at[r, h, yq], r_xb.at[r, h, yq], xdev,
        )

    def xa_copy(r, h):
        return send(
            ya.at[2 * r + 1 - x, band(h)], xa.at[r, band(h)], s_xa.at[r, h], r_xa.at[r, h], xdev
        )

    def yb_copy(r, h):
        return send(
            xb.at[r, band(h), span((1 - y) * eighth, eighth)],
            yb.at[r, band(h)], s_yb.at[r, h], r_yb.at[r, h], ydev,
        )

    def z_copy(r, h):
        return send(
            own.at[r, band(h)], zin.at[z, band(h)], s_z.at[r, h], r_z.at[z, h],
            {"ep": 2 * r + x, "tp": tp},
        )

    def z_wait(origin, h):
        return send(
            own.at[origin, band(h)], zin.at[origin, band(h)], s_z.at[0, h], r_z.at[origin, h],
            {"ep": 2 * origin + x, "tp": tp},
        )

    def add(a, b):
        return (a.astype(jnp.float32) + b.astype(jnp.float32)).astype(jnp.bfloat16)

    ff = gate_w.shape[1]
    fstep = min(256, ff)

    def lift(items):
        total = len(items) * rows

        def lhs_of():
            return jnp.concatenate([gath[b, band(h), :] for b, h in items], axis=0)

        for k, (b, h) in enumerate(items):
            line = gtab[b, :, h * rows:(h + 1) * rows]
            route_buf[k * rows:(k + 1) * rows, :] = jnp.transpose(jnp.broadcast_to(line, (128, rows)))
        route = jnp.concatenate([route_buf[0:total, :]] * (fstep // 128), axis=1)

        def ff_step(j, carry):
            at = span(j * fstep, fstep)
            lhs = lhs_of()
            gate = jnp.dot(lhs, gate_w[:, at], preferred_element_type=jnp.float32)
            upper = jnp.dot(lhs, up_w[:, at], preferred_element_type=jnp.float32)
            value = activate(gate, upper)
            hidden[0:total, at] = jnp.where(route > 0, route * value, 0.0).astype(jnp.bfloat16)
            return carry

        lax.fori_loop(0, ff // fstep, ff_step, 0)

    def lower(items):
        total = len(items) * rows

        def down_step(j, carry):
            yq = j % 2
            cc = jnp.where(j < 2, 1 - c, c)
            at = span((2 * yq + cc) * quarter, quarter)
            value = jnp.dot(hidden[0:total, :], down_w[:, at], preferred_element_type=jnp.float32)
            value = value.astype(jnp.bfloat16)
            for k, (b, h) in enumerate(items):
                part[b, band(h), at] = value[k * rows:(k + 1) * rows]

            @pl.when(j < 2)
            def _():
                for b, h in items:
                    d_copy(b, h, yq, 1 - c).start()

            return carry

        lax.fori_loop(0, 4, down_step, 0)

    def raw_copy(r, h):
        return send(
            dbuf.at[pl.ds(2 * r, 2), band(h)], raw.at[:, band(h)],
            s_raw.at[h], r_raw.at[h], inward,
        )

    def stage_a(r, h, joined, passed_on):
        if joined:
            raw_copy(r, h).wait_recv()
        for j in (0, 1):
            for yq in (0, 1):
                b = 2 * r + j
                d_copy(b, h, yq, 1 - c).wait_recv()
                at = span(yq * quarter, quarter)
                total = part[b, band(h), span((2 * yq + c) * quarter, quarter)].astype(jnp.float32)
                total = total + dbuf[b, band(h), at].astype(jnp.float32)
                if joined:
                    total = total + raw[j, band(h), at].astype(jnp.float32)
                dbuf[b, band(h), at] = total.astype(jnp.bfloat16)
        if passed_on:
            raw_copy(r, h).start()
            return
        ya_copy(r, h).start()
        for yq in (0, 1):
            xb_copy(r, h, yq).start()

    def stage_ba(r, h):
        ya_copy(r, h).wait_recv()
        pair = pl.ds(2 * r, 2)
        ya[pair, band(h)] = add(dbuf[pair, band(h), span(y * quarter, eighth)], ya[pair, band(h)])
        xa_copy(r, h).start()

    def stage_bb(r, h):
        for yq in (0, 1):
            xb_copy(r, h, yq).wait_recv()
            at = span(yq * eighth, eighth)
            kept = dbuf[2 * r + x, band(h), span(yq * quarter + eighth, eighth)]
            xb[r, band(h), at] = add(kept, xb[r, band(h), at])
        yb_copy(r, h).start()

    def stage_c(r, h, leave):
        xa_copy(r, h).wait_recv()
        own[r, band(h), 0:eighth] = add(ya[2 * r + x, band(h)], xa[r, band(h)])
        yb_copy(r, h).wait_recv()
        own[r, band(h), eighth:quarter] = add(
            xb[r, band(h), span(y * eighth, eighth)], yb[r, band(h)]
        )
        if leave:
            z_copy(r, h).start()

    def settle(h, origins):
        total = own[z, band(h)].astype(jnp.float32)
        for origin in origins:
            z_wait(origin, h).wait_recv()
            total = total + zin[origin, band(h)].astype(jnp.float32)
        out_ref[band(h), :] = total.astype(jnp.bfloat16)

    def wait_weights():
        for item in weight_copies:
            item.wait()

    def drive(order, end):
        planes = [z + toward * k for k in ((0, 1, 2, 3) if end else (0, -1, 1, 2))]
        state = {"tables": False}

        def block_of(q, flip):
            return 2 * planes[q] + (x if flip == 0 else 1 - x)

        def on_p(q, flip, h):
            block = block_of(q, flip)
            got(block, h)
            if q > 0 and not end and (flip == 0 or XZ[h]):
                go_z(block, h, 0 if q == 1 else 1).start()
            if q > 0 and flip == 0 and not XZ[h]:
                go_x(block, h).start()
            if q == 0 and XZ[h]:
                go_z(block, h, 0).start()
                if not end:
                    go_z(block, h, 1).start()
            spread(block, h)

        def gather_sends(q):
            for flip in (0, 1):
                for h in range(pieces):
                    block = block_of(q, flip)
                    if flip == 0 and (q == 0 or not XZ[h]):
                        go_x(block, h).wait_send()
                    if flip == 0 or XZ[h]:
                        if q == 0 or (q == 1 and not end):
                            go_z(block, h, 0).wait_send()
                        if q != 1 and not end:
                            go_z(block, h, 1).wait_send()
                    if q > 0 or flip == 1:
                        go_y(block, h, y).wait_send()
                        for kind in (0, 1):
                            go_d(block, h, kind, c).wait_send()

        def rest_sends(q):
            r = planes[q]
            for h in range(pieces):
                for yq in (0, 1):
                    for b in (2 * r, 2 * r + 1):
                        d_copy(b, h, yq, 1 - c).wait_send()
                if end and q == 1:
                    raw_copy(r, h).wait_send()
                    continue
                for yq in (0, 1):
                    xb_copy(r, h, yq).wait_send()
                ya_copy(r, h).wait_send()
                xa_copy(r, h).wait_send()
                yb_copy(r, h).wait_send()

        def items_of(q, h):
            if h < 0:
                return [(mine if h == -1 else other, g) for g in range(pieces)]
            return [(2 * planes[q], h), (2 * planes[q] + 1, h)]

        for op, q, *rest in order:
            if op == "P":
                on_p(q, *rest)
            elif op == "Y":
                on_y(block_of(q, rest[0]), rest[1])
            elif op == "F":
                if rest[0] == -1:
                    wait_weights()
                else:
                    if not state["tables"]:
                        for k in range(1, n_ep):
                            table_wait(lax.rem(ep + k, n_ep)).wait_recv()
                        state["tables"] = True
                    for block, h in items_of(q, rest[0]):
                        ready(block, h)
                lift(items_of(q, rest[0]))
            elif op == "N":
                lower(items_of(q, rest[0]))
            elif op == "A":
                stage_a(planes[q], rest[0], not end and q == 0, end and q == 1)
            elif op == "Ba":
                stage_ba(planes[q], rest[0])
            elif op == "Bb":
                stage_bb(planes[q], rest[0])
            elif op == "C":
                stage_c(planes[q], rest[0], q > 0)
            elif op == "S":
                settle(q, planes[1:] if end else planes[2:])
            elif op == "W":
                (rest_sends if rest[0] else gather_sends)(q)
        for q in range(1, 4):
            for h in range(pieces):
                if end and q == 1:
                    continue
                z_copy(planes[q], h).wait_send()

    @pl.when(at_end)
    def _():
        drive(END, True)

    @pl.when(~at_end)
    def _():
        drive(MIDDLE, False)

    for k in range(1, n_ep):
        table(k).wait_send()


def dense(tokens, norm_gain, expert_ids, route_weights, gate_weight, up_weight, down_weight):
    rows, width = tokens.shape
    n_ep = lax.axis_size("ep")
    nz = n_ep // 2
    pieces = len(XZ)
    ff = gate_weight.shape[2]
    quarter = width // lax.axis_size("tp")
    eighth = quarter // 2
    onehot = expert_ids[:, :, None] == jnp.arange(n_ep, dtype=jnp.int32)[None, None, :]
    table = jnp.sum(jnp.where(onehot, route_weights[:, :, None], 0.0), axis=1)
    vmem = pl.BlockSpec(memory_space=pltpu.VMEM)
    hbm = pl.BlockSpec(memory_space=pl.ANY)
    bf16 = jnp.bfloat16
    dma = pltpu.SemaphoreType.DMA
    return pl.pallas_call(
        functools.partial(kernel, n_ep),
        out_shape=jax.ShapeDtypeStruct((rows, quarter), bf16),
        in_specs=[vmem, vmem, vmem, hbm, hbm, hbm],
        out_specs=vmem,
        scratch_shapes=[
            pltpu.VMEM((n_ep, rows, width), bf16),
            pltpu.VMEM((n_ep, 1, rows), jnp.float32),
            pltpu.VMEM((rows, 128), jnp.float32),
            pltpu.VMEM((width, ff), bf16),
            pltpu.VMEM((width, ff), bf16),
            pltpu.VMEM((ff, width), bf16),
            pltpu.VMEM((rows, ff), bf16),
            pltpu.VMEM((n_ep, rows, width), bf16),
            pltpu.VMEM((n_ep, rows, 2 * quarter), bf16),
            pltpu.VMEM((n_ep, rows, eighth), bf16),
            pltpu.VMEM((nz, rows, eighth), bf16),
            pltpu.VMEM((nz, rows, 2 * eighth), bf16),
            pltpu.VMEM((nz, rows, eighth), bf16),
            pltpu.VMEM((nz, rows, quarter), bf16),
            pltpu.VMEM((nz, rows, quarter), bf16),
            pltpu.VMEM((2, rows, 2 * quarter), bf16),
            dma((3,)),
            dma((n_ep,)), dma((n_ep,)),
            dma((n_ep, pieces)),
            dma((2, n_ep, pieces)), dma((n_ep, pieces)),
            dma((n_ep, pieces)), dma((n_ep, pieces)),
            dma((2, n_ep, pieces)), dma((2, n_ep, pieces)),
            dma((n_ep, pieces, 2)), dma((n_ep, pieces, 2)),
            dma((nz, pieces)), dma((nz, pieces)),
            dma((nz, pieces, 2)), dma((nz, pieces, 2)),
            dma((nz, pieces)), dma((nz, pieces)),
            dma((nz, pieces)), dma((nz, pieces)),
            dma((nz, pieces)), dma((nz, pieces)),
            dma((pieces,)), dma((pieces,)),
        ],
        compiler_params=pltpu.CompilerParams(
            collective_id=0, has_side_effects=True, vmem_limit_bytes=60 * 1024 * 1024
        ),
    )(tokens, norm_gain[None, :], table.T[:, None, :], gate_weight, up_weight, down_weight)


def per_device(tokens, norm_gain, expert_ids, route_weights, gate_weight, up_weight, down_weight):
    tok_dev, top = expert_ids.shape
    experts = gate_weight.shape[0] * lax.axis_size("ep")
    whole = gate_weight.shape[0] == 1 and 2 * tok_dev * top // experts >= tok_dev
    whole = whole and lax.axis_size("tp") == 4 and lax.axis_size("ep") == 8
    form = dense if whole and tokens.shape[1] % 2048 == 0 else routed
    return form(
        tokens, norm_gain, expert_ids, route_weights, gate_weight, up_weight, down_weight
    )


def solution(mesh):
    in_specs = (
        P("ep", None),
        P(),
        P("ep", None),
        P("ep", None),
        P("ep", None, "tp"),
        P("ep", None, "tp"),
        P("ep", "tp", None),
    )
    return jax.shard_map(
        per_device, mesh=mesh, in_specs=in_specs, out_specs=P("ep", "tp"), check_vma=False
    )
```

```python
import functools

import jax
import jax.numpy as jnp
from jax import lax
from jax.experimental import pallas as pl
from jax.experimental.pallas import tpu as pltpu
from jax.sharding import PartitionSpec as P


MESH = pl.DeviceIdType.MESH


def normalise(tokens, norm_gain):
    values = tokens.astype(jnp.float32)
    scale = lax.rsqrt(jnp.mean(values * values, axis=1, keepdims=True) + 1e-06)
    return (values * scale * norm_gain[None, :]).astype(jnp.bfloat16)


def activate(gate, upper):
    gate = jnp.minimum(gate, 7.0)
    upper = jnp.clip(upper, -7.0, 7.0)
    return (upper + 1.0) * (gate * jax.nn.sigmoid(1.702 * gate))


def routed(tokens, norm_gain, expert_ids, route_weights, gate_weight, up_weight, down_weight):
    tok_dev, width = tokens.shape
    top = expert_ids.shape[1]
    n_ep = lax.axis_size("ep")
    n_tp = lax.axis_size("tp")
    exp_dev = gate_weight.shape[0]
    experts = exp_dev * n_ep
    capacity = 2 * tok_dev * top // experts
    quarter = width // n_tp
    normed = normalise(tokens, norm_gain)
    flat = expert_ids.reshape(-1)
    count = flat.shape[0]
    onehot = (flat[:, None] == jnp.arange(experts, dtype=jnp.int32)[None, :]).astype(jnp.int32)
    before = jnp.cumsum(onehot, axis=0) - onehot
    slot = jnp.sum(before * onehot, axis=1)
    position = flat * capacity + slot
    source_tok = jnp.arange(count, dtype=jnp.int32) // top
    buffer_tok = jnp.zeros((experts * capacity,), jnp.int32).at[position].set(source_tok)
    buffer_live = jnp.zeros((experts * capacity,), jnp.int32).at[position].set(1)
    columns = lax.dynamic_slice_in_dim(normed, lax.axis_index("tp") * quarter, quarter, 1)
    outgoing = jnp.where(buffer_live[:, None] > 0, columns[buffer_tok], jnp.zeros((), jnp.bfloat16))
    outgoing = outgoing.reshape(n_ep, exp_dev, capacity, quarter)
    received = lax.all_gather(
        lax.all_to_all(outgoing, "ep", split_axis=0, concat_axis=0, tiled=True),
        "tp",
        axis=3,
        tiled=True,
    )
    gate = jnp.einsum("sxcd,xdf->sxcf", received, gate_weight, preferred_element_type=jnp.float32)
    upper = jnp.einsum("sxcd,xdf->sxcf", received, up_weight, preferred_element_type=jnp.float32)
    hidden = activate(gate, upper).astype(jnp.bfloat16)
    partial_value = jnp.einsum(
        "sxcf,xfd->sxcd", hidden, down_weight, preferred_element_type=jnp.float32
    )
    rounded = partial_value.astype(jnp.bfloat16)
    summed = lax.psum_scatter(rounded, "tp", scatter_dimension=3, tiled=True)
    returned = lax.all_to_all(summed, "ep", split_axis=0, concat_axis=0, tiled=True)
    returned = returned.reshape(experts * capacity, quarter)
    picked = returned[position].reshape(tok_dev, top, quarter)
    mixed = jnp.sum(route_weights[:, :, None] * picked.astype(jnp.float32), axis=1)
    return mixed.astype(jnp.bfloat16)


XZ = (False, False, True, True)
SPECIAL = 8
END = (
    ("F", 0, -1), ("N", 0, -1), ("P", 0, 1, 3), ("P", 1, 0, 0), ("P", 0, 1, 2),
    ("P", 1, 0, 1), ("Y", 0, 1, 3), ("Y", 1, 0, 0), ("P", 0, 1, 1), ("P", 1, 0, 2),
    ("Y", 0, 1, 2), ("Y", 1, 0, 1), ("P", 0, 1, 0), ("P", 1, 0, 3), ("Y", 0, 1, 1),
    ("Y", 1, 0, 2), ("P", 1, 1, 0), ("P", 2, 0, 0), ("Y", 0, 1, 0), ("Y", 1, 0, 3),
    ("F", 0, -2), ("P", 1, 1, 3), ("Y", 1, 1, 0), ("P", 1, 1, 1), ("N", 0, -2),
    ("P", 1, 1, 2), ("F", 1, 0), ("A", 0, 0), ("A", 0, 2), ("Y", 1, 1, 3),
    ("P", 2, 1, 0), ("A", 0, 1), ("N", 1, 0), ("Y", 1, 1, 2), ("P", 2, 0, 1),
    ("F", 1, 3), ("A", 1, 0), ("P", 2, 0, 2), ("N", 1, 3), ("Bb", 0, 0),
    ("Y", 2, 0, 0), ("Y", 1, 1, 1), ("A", 1, 3), ("Ba", 0, 2), ("Bb", 0, 2),
    ("Ba", 0, 0), ("P", 2, 0, 3), ("F", 1, 2), ("Y", 2, 1, 0), ("N", 1, 2),
    ("Bb", 0, 1), ("Ba", 0, 1), ("F", 1, 1), ("P", 2, 1, 1), ("Y", 2, 0, 2),
    ("P", 2, 1, 3), ("N", 1, 1), ("P", 3, 0, 0), ("F", 2, 0), ("C", 0, 0),
    ("A", 1, 1), ("C", 0, 2), ("Y", 2, 0, 3), ("N", 2, 0), ("P", 2, 1, 2),
    ("C", 0, 1), ("Y", 2, 1, 1), ("A", 1, 2), ("A", 2, 0), ("Y", 2, 0, 1),
    ("Y", 2, 1, 3), ("P", 3, 0, 1), ("P", 3, 1, 0), ("Y", 3, 0, 0), ("F", 2, 1),
    ("Y", 2, 1, 2), ("N", 2, 1), ("P", 3, 0, 2), ("Bb", 2, 0), ("F", 2, 2),
    ("A", 2, 1), ("N", 2, 2), ("P", 3, 1, 1), ("P", 3, 0, 3), ("Y", 3, 1, 0),
    ("Ba", 2, 0), ("Y", 3, 0, 2), ("Y", 3, 0, 1), ("F", 2, 3), ("A", 2, 2),
    ("N", 2, 3), ("P", 3, 1, 3), ("Bb", 2, 1), ("F", 3, 0), ("A", 2, 3),
    ("Y", 3, 1, 1), ("P", 3, 1, 2), ("C", 2, 0), ("Ba", 2, 1), ("N", 3, 0),
    ("Bb", 2, 2), ("Y", 3, 0, 3), ("A", 3, 0), ("Y", 3, 1, 3), ("Ba", 2, 2),
    ("A", 0, 3), ("F", 3, 1), ("Bb", 2, 3), ("C", 2, 1), ("N", 3, 1),
    ("Ba", 2, 3), ("F", 3, 3), ("A", 3, 1), ("Bb", 3, 0), ("C", 2, 2),
    ("N", 3, 3), ("Y", 3, 1, 2), ("Ba", 3, 0), ("Bb", 0, 3), ("A", 3, 3),
    ("Ba", 0, 3), ("F", 3, 2), ("C", 2, 3), ("N", 3, 2), ("Ba", 3, 1),
    ("Bb", 3, 1), ("C", 3, 0), ("A", 3, 2), ("Bb", 3, 3), ("C", 0, 3),
    ("Ba", 3, 3), ("C", 3, 1), ("Ba", 3, 2), ("Bb", 3, 2), ("C", 3, 3),
    ("S", 0), ("C", 3, 2), ("S", 1), ("S", 3), ("S", 2),
)
MIDDLE = (
    ("F", 0, -1), ("N", 0, -1), ("P", 2, 0, 0), ("P", 0, 1, 3), ("P", 1, 0, 0),
    ("P", 0, 1, 2), ("P", 2, 0, 1), ("P", 1, 0, 1), ("Y", 2, 0, 0), ("Y", 0, 1, 3),
    ("Y", 1, 0, 0), ("P", 0, 1, 1), ("P", 2, 0, 2), ("P", 1, 0, 2), ("Y", 0, 1, 2),
    ("Y", 2, 0, 1), ("Y", 1, 0, 1), ("P", 0, 1, 0), ("P", 1, 0, 3), ("P", 2, 0, 3),
    ("Y", 0, 1, 1), ("Y", 2, 0, 2), ("Y", 1, 0, 2), ("P", 1, 1, 3), ("P", 2, 1, 0),
    ("P", 2, 1, 3), ("Y", 0, 1, 0), ("Y", 1, 0, 3), ("F", 0, -2), ("P", 1, 1, 2),
    ("P", 3, 0, 0), ("P", 1, 1, 0), ("Y", 1, 1, 3), ("N", 0, -2), ("Y", 2, 1, 3),
    ("P", 2, 1, 2), ("F", 1, 3), ("Y", 2, 1, 0), ("P", 2, 1, 1), ("N", 1, 3),
    ("P", 3, 0, 1), ("Y", 3, 0, 0), ("P", 1, 1, 1), ("Y", 2, 0, 3), ("Y", 1, 1, 2),
    ("F", 2, 0), ("A", 1, 3), ("Y", 1, 1, 0), ("Y", 2, 1, 2), ("N", 2, 0),
    ("P", 3, 0, 2), ("Y", 3, 0, 1), ("Y", 2, 1, 1), ("P", 3, 1, 0), ("F", 2, 3),
    ("Y", 1, 1, 1), ("A", 2, 0), ("P", 3, 1, 1), ("P", 3, 0, 3), ("N", 2, 3),
    ("F", 2, 1), ("Bb", 1, 3), ("Y", 3, 0, 2), ("P", 3, 1, 3), ("A", 2, 3),
    ("Ba", 1, 3), ("Y", 3, 1, 0), ("N", 2, 1), ("Ba", 2, 0), ("Bb", 2, 0),
    ("F", 3, 0), ("P", 3, 1, 2), ("Y", 3, 1, 1), ("A", 2, 1), ("Y", 3, 0, 3),
    ("N", 3, 0), ("F", 1, 1), ("Y", 3, 1, 3), ("C", 1, 3), ("A", 3, 0),
    ("Bb", 2, 3), ("N", 1, 1), ("Bb", 2, 1), ("Ba", 2, 3), ("F", 3, 3),
    ("C", 2, 0), ("A", 1, 1), ("Y", 3, 1, 2), ("N", 3, 3), ("Bb", 3, 0),
    ("F", 3, 2), ("Ba", 3, 0), ("A", 3, 3), ("N", 3, 2), ("Bb", 1, 1),
    ("Ba", 2, 1), ("F", 1, 0), ("A", 3, 2), ("Ba", 1, 1), ("N", 1, 0),
    ("C", 3, 0), ("C", 2, 3), ("A", 1, 0), ("Bb", 3, 3), ("C", 2, 1),
    ("A", 0, 1), ("Ba", 3, 3), ("F", 3, 1), ("N", 3, 1), ("Ba", 3, 2),
    ("C", 1, 1), ("Bb", 3, 2), ("A", 3, 1), ("Ba", 1, 0), ("Bb", 1, 0),
    ("F", 2, 2), ("Bb", 0, 1), ("N", 2, 2), ("A", 0, 2), ("Ba", 0, 1),
    ("A", 2, 2), ("C", 3, 2), ("C", 3, 3), ("F", 1, 2), ("C", 1, 0),
    ("Bb", 3, 1), ("N", 1, 2), ("Ba", 3, 1), ("Bb", 0, 2), ("Ba", 0, 2),
    ("A", 1, 2), ("C", 0, 1), ("S", 1), ("A", 0, 3), ("A", 0, 0),
    ("Bb", 2, 2), ("Ba", 2, 2), ("C", 3, 1), ("C", 0, 2), ("Bb", 1, 2),
    ("Ba", 1, 2), ("Bb", 0, 3), ("Ba", 0, 3), ("Bb", 0, 0), ("Ba", 0, 0),
    ("C", 2, 2), ("C", 1, 2), ("C", 0, 3), ("C", 0, 0), ("S", 0),
    ("S", 3), ("S", 2),
)


def kernel(
    n_ep, tokens_hbm, gain_ref, ids_ref, mix_ref, gate_hbm, up_hbm, down_hbm, out_ref,
    tokens_ref, gath, gtab, route_buf, gate_w, up_w, down_w, hidden, part, dbuf,
    ya, xa, xb, yb, own, zin, raw,
    t_sem, w_sem, gone, st, rt, rp, ry, rg, r_d, r_ya, r_xb, r_xa, r_yb, r_z, r_raw,
):
    ep, tp = lax.axis_index("ep"), lax.axis_index("tp")
    z, x, y, c = ep // 2, ep % 2, tp // 2, tp % 2
    nz = n_ep // 2
    width = tokens_ref.shape[1]
    quarter = width // 4
    eighth = quarter // 2
    side = width // 2
    special = width // SPECIAL
    primary = side - special
    pieces = len(XZ)
    rows = tokens_ref.shape[0] // pieces
    mine, other = ep, 2 * z + 1 - x
    toward = jnp.where(z < nz // 2, 1, -1)
    at_end = (z == 0) | (z == nz - 1)
    inward = {"ep": lax.rem(ep + 2 * toward + n_ep, n_ep), "tp": tp}
    outward = {"ep": lax.rem(ep - 2 * toward + n_ep, n_ep), "tp": tp}
    xdev = {"ep": other, "tp": tp}
    ydev = {"ep": ep, "tp": 2 * (1 - y) + c}
    ddev = {"ep": ep, "tp": 2 * y + 1 - c}

    barrier = pltpu.get_barrier_semaphore()

    def greet(device):
        pl.semaphore_signal(barrier, inc=1, device_id=device, device_id_type=MESH)

    for device in (xdev, ydev, ddev, inward):
        greet(device)

    @pl.when(~at_end)
    def _():
        greet(outward)

    def load(h):
        at = pl.ds(h * rows, rows)
        return pltpu.make_async_copy(tokens_hbm.at[at], tokens_ref.at[at], t_sem.at[h])

    weight_copies = [
        pltpu.make_async_copy(gate_hbm.at[0], gate_w, w_sem.at[0]),
        pltpu.make_async_copy(up_hbm.at[0], up_w, w_sem.at[1]),
        pltpu.make_async_copy(down_hbm.at[0], down_w, w_sem.at[2]),
    ]
    slow_first = [h for h in range(pieces) if not XZ[h]] + [h for h in range(pieces) if XZ[h]]
    norm_order = []
    for h in range((pieces + 1) // 2):
        for g in (slow_first[-1 - h], slow_first[h]):
            if g not in norm_order:
                norm_order.append(g)
    for h in norm_order:
        load(h).start()
    for item in weight_copies:
        item.start()

    tile = 32

    def normalise_piece(h):
        load(h).wait()

        def norm_step(i, carry):
            at = pl.ds(pl.multiple_of(h * rows + i * tile, tile), tile)
            values = tokens_ref[at, :].astype(jnp.float32)
            scale = lax.rsqrt(jnp.mean(values * values, axis=1, keepdims=True) + 1e-06)
            gath[ep, at, :] = (values * scale * gain_ref[...]).astype(jnp.bfloat16)
            return carry

        lax.fori_loop(0, rows // tile, norm_step, 0)

    def span(start, size):
        return pl.ds(pl.multiple_of(start, 128), size)

    def send(src, dst, send_sem, recv_sem, device):
        return pltpu.make_async_remote_copy(
            src_ref=src, dst_ref=dst, send_sem=send_sem, recv_sem=recv_sem,
            device_id=device, device_id_type=MESH,
        )

    def band(h):
        start = h * rows
        return pl.ds(start if isinstance(start, int) else pl.multiple_of(start, 16), rows)

    def move(block, h, start, size, device, send_sem, recv_sem):
        ref = gath.at[block, band(h), span(start, size)]
        return send(ref, ref, send_sem, recv_sem, device)

    def go_main(block, h, device, send_sem):
        return move(block, h, c * side + y * special, primary, device, send_sem, rp.at[block, h])

    def go_z(block, h, way):
        return go_main(block, h, inward if way == 0 else outward, gone.at[1 + way, block // 2])

    def go_x(block, h):
        return go_main(block, h, xdev, gone.at[0, block // 2])

    def go_y(block, h, yy):
        start = c * side + yy * primary
        return move(block, h, start, special, ydev, gone.at[3, block // 2], ry.at[block, h])

    def go_d(block, h, kind, cc):
        start = cc * side + (y * special if kind == 0 else (1 - y) * primary)
        size = primary if kind == 0 else special
        plane, turn = block // 2, jnp.where(block // 2 == z, 0, h)
        return move(block, h, start, size, ddev, gone.at[4, plane], rg.at[plane, turn])

    def go_table(block, path):
        device = (xdev, inward, outward)[path]
        return send(gtab.at[block], gtab.at[block], st.at[path, block], rt.at[block], device)

    def drain(kind, plane, elements):
        for blocks in range(n_ep, 0, -1):
            lanes, left = divmod(elements, blocks * pieces * rows)
            if left == 0 and lanes % 128 == 0 and lanes <= width:
                ref = gath.at[pl.ds(0, blocks), :, pl.ds(0, lanes)]
                send(ref, ref, gone.at[kind, plane], rt.at[0], xdev).wait_send()
                return
        raise ValueError("size")

    def first_x(h):
        go_x(mine, h).start()

    def first_z(h):
        go_z(mine, h, 0).start()

        @pl.when(~at_end)
        def _():
            go_z(mine, h, 1).start()

    expert = lax.broadcasted_iota(jnp.int32, (n_ep, pieces * rows), 0)
    mixing = jnp.zeros((n_ep, pieces * rows), jnp.float32)
    for k in range(ids_ref.shape[0]):
        mixing = mixing + jnp.where(ids_ref[k:k + 1, :] == expert, mix_ref[k:k + 1, :], 0.0)
    gtab[ep] = mixing

    x_left, z_left = slow_first[::-1], list(slow_first)
    settled = []
    for h in norm_order:
        normalise_piece(h)
        if not settled:
            pl.semaphore_wait(barrier, jnp.where(at_end, 4, 5))
            go_table(mine, 0).start()
            go_table(mine, 1).start()

            @pl.when(~at_end)
            def _():
                go_table(mine, 2).start()

        settled.append(h)
        while x_left and x_left[0] in settled:
            first_x(x_left.pop(0))
        while z_left and z_left[0] in settled:
            first_z(z_left.pop(0))

    def got(block, h):
        go_x(block, h).wait_recv()

    def spread(block, h):
        go_y(block, h, y).start()
        go_d(block, h, 0, c).start()

    def on_y(block, h):
        go_y(block, h, 1 - y).wait_recv()
        go_d(block, h, 1, c).start()

    def ready_own():
        ref = gath.at[other, :, span((1 - c) * side, side)]
        send(ref, ref, gone.at[4, 0], rg.at[z, 0], ddev).wait_recv()

    def ready(r, h):
        ref = gath.at[pl.ds(2 * r, 2), band(h), span((1 - c) * side, side)]
        send(ref, ref, gone.at[4, 0], rg.at[r, h], ddev).wait_recv()

    def d_copy(b, h, yq, cc):
        return send(
            part.at[b, band(h), span((2 * yq + cc) * quarter, quarter)],
            dbuf.at[b, band(h), span(yq * quarter, quarter)],
            gone.at[6, b // 2], r_d.at[b // 2, h], ddev,
        )

    def ya_copy(r, h):
        return send(
            dbuf.at[pl.ds(2 * r, 2), band(h), span((1 - y) * quarter, eighth)],
            ya.at[pl.ds(2 * r, 2), band(h)], gone.at[7, r], r_ya.at[r, h], ydev,
        )

    def xb_copy(r, h, yq):
        return send(
            dbuf.at[2 * r + 1 - x, band(h), span(yq * quarter + eighth, eighth)],
            xb.at[r, band(h), span(yq * eighth, eighth)],
            gone.at[8, r], r_xb.at[r, h], xdev,
        )

    def xa_copy(r, h):
        return send(
            ya.at[2 * r + 1 - x, band(h)], xa.at[r, band(h)], gone.at[9, r], r_xa.at[r, h], xdev
        )

    def yb_copy(r, h):
        return send(
            xb.at[r, band(h), span((1 - y) * eighth, eighth)],
            yb.at[r, band(h)], gone.at[10, r], r_yb.at[r, h], ydev,
        )

    def z_copy(r, h):
        return send(
            own.at[r, band(h)], zin.at[z, band(h)], gone.at[11, 0], r_z.at[h],
            {"ep": 2 * r + x, "tp": tp},
        )

    def z_wait(count, h):
        ref = zin.at[pl.ds(0, count), band(h)]
        send(ref, ref, gone.at[11, 0], r_z.at[h], inward).wait_recv()

    def add(a, b):
        return (a.astype(jnp.float32) + b.astype(jnp.float32)).astype(jnp.bfloat16)

    ff = gate_w.shape[1]
    fstep = min(256, ff)

    def lift(items):
        total = len(items) * rows

        def lhs_of():
            return jnp.concatenate([gath[b, band(h), :] for b, h in items], axis=0)

        for k, (b, h) in enumerate(items):
            lines = gtab[b, :, h * rows:(h + 1) * rows]
            chosen = lax.broadcasted_iota(jnp.int32, lines.shape, 0) == ep
            line = jnp.sum(jnp.where(chosen, lines, 0.0), axis=0, keepdims=True)
            route_buf[k * rows:(k + 1) * rows, :] = jnp.transpose(jnp.broadcast_to(line, (128, rows)))
        route = jnp.concatenate([route_buf[0:total, :]] * (fstep // 128), axis=1)

        def ff_step(j, carry):
            at = span(j * fstep, fstep)
            lhs = lhs_of()
            gate = jnp.dot(lhs, gate_w[:, at], preferred_element_type=jnp.float32)
            upper = jnp.dot(lhs, up_w[:, at], preferred_element_type=jnp.float32)
            value = activate(gate, upper)
            hidden[0:total, at] = jnp.where(route > 0, route * value, 0.0).astype(jnp.bfloat16)
            return carry

        lax.fori_loop(0, ff // fstep, ff_step, 0)

    def lower(items):
        total = len(items) * rows

        def down_step(j, carry):
            yq = j % 2
            cc = jnp.where(j < 2, 1 - c, c)
            at = span((2 * yq + cc) * quarter, quarter)
            value = jnp.dot(hidden[0:total, :], down_w[:, at], preferred_element_type=jnp.float32)
            value = value.astype(jnp.bfloat16)
            for k, (b, h) in enumerate(items):
                part[b, band(h), at] = value[k * rows:(k + 1) * rows]

            @pl.when(j < 2)
            def _():
                for b, h in items:
                    d_copy(b, h, yq, 1 - c).start()

            return carry

        lax.fori_loop(0, 4, down_step, 0)

    def raw_copy(r, h):
        return send(
            dbuf.at[pl.ds(2 * r, 2), band(h)], raw.at[:, band(h)],
            gone.at[12, 0], r_raw.at[h], inward,
        )

    def stage_a(r, h, joined, passed_on):
        if joined:
            raw_copy(r, h).wait_recv()
        both = dbuf.at[pl.ds(2 * r, 2), band(h)]
        send(both, both, gone.at[6, 0], r_d.at[r, h], ddev).wait_recv()
        for j in (0, 1):
            for yq in (0, 1):
                b = 2 * r + j
                at = span(yq * quarter, quarter)
                total = part[b, band(h), span((2 * yq + c) * quarter, quarter)].astype(jnp.float32)
                total = total + dbuf[b, band(h), at].astype(jnp.float32)
                if joined:
                    total = total + raw[j, band(h), at].astype(jnp.float32)
                dbuf[b, band(h), at] = total.astype(jnp.bfloat16)
        if passed_on:
            raw_copy(r, h).start()
            return
        ya_copy(r, h).start()
        for yq in (0, 1):
            xb_copy(r, h, yq).start()

    def stage_ba(r, h):
        ya_copy(r, h).wait_recv()
        pair = pl.ds(2 * r, 2)
        ya[pair, band(h)] = add(dbuf[pair, band(h), span(y * quarter, eighth)], ya[pair, band(h)])
        xa_copy(r, h).start()

    def stage_bb(r, h):
        landed = xb.at[r, band(h)]
        send(landed, landed, gone.at[8, r], r_xb.at[r, h], xdev).wait_recv()
        for yq in (0, 1):
            at = span(yq * eighth, eighth)
            kept = dbuf[2 * r + x, band(h), span(yq * quarter + eighth, eighth)]
            xb[r, band(h), at] = add(kept, xb[r, band(h), at])
        yb_copy(r, h).start()

    def stage_c(r, h, leave):
        xa_copy(r, h).wait_recv()
        own[r, band(h), 0:eighth] = add(ya[2 * r + x, band(h)], xa[r, band(h)])
        yb_copy(r, h).wait_recv()
        own[r, band(h), eighth:quarter] = add(
            xb[r, band(h), span(y * eighth, eighth)], yb[r, band(h)]
        )
        if leave:
            z_copy(r, h).start()

    def settle(h, origins):
        total = own[z, band(h)].astype(jnp.float32)
        z_wait(len(origins), h)
        for origin in origins:
            total = total + zin[origin, band(h)].astype(jnp.float32)
        out_ref[band(h), :] = total.astype(jnp.bfloat16)

    def wait_weights():
        for item in weight_copies:
            item.wait()

    def drive(order, end):
        planes = [z + toward * k for k in ((0, 1, 2, 3) if end else (0, -1, 1, 2))]
        told = set()

        def block_of(q, flip):
            return 2 * planes[q] + (x if flip == 0 else 1 - x)

        def on_p(q, flip, h):
            block = block_of(q, flip)
            got(block, h)
            if (q, flip) not in told:
                told.add((q, flip))
                go_table(block, 0).wait_recv()
                if q > 0 and flip == 0:
                    if not end:
                        go_table(block, 1 if q == 1 else 2).start()
                    go_table(block, 0).start()
            if q > 0 and not end and (flip == 0 or XZ[h]):
                go_z(block, h, 0 if q == 1 else 1).start()
            if q > 0 and flip == 0 and not XZ[h]:
                go_x(block, h).start()
            if q == 0 and XZ[h]:
                go_z(block, h, 0).start()
                if not end:
                    go_z(block, h, 1).start()
            spread(block, h)

        def drain_all():
            piece = rows * primary
            slow = len([h for h in range(pieces) if not XZ[h]])
            crossed = 2 * pieces - slow
            whole_rows = pieces * rows
            for q in range(4):
                r, blocks = planes[q], 1 if q == 0 else 2
                drain(0, r, (pieces if q == 0 else slow) * piece)
                if q == 0 or (q == 1 and not end):
                    drain(1, r, crossed * piece)
                if q != 1 and not end:
                    drain(2, r, crossed * piece)
                drain(3, r, blocks * whole_rows * special)
                drain(4, r, blocks * whole_rows * side)
                drain(6, r, 2 * whole_rows * side)
                if end and q == 1:
                    continue
                drain(7, r, 2 * whole_rows * eighth)
                drain(8, r, whole_rows * quarter)
                drain(9, r, whole_rows * eighth)
                drain(10, r, whole_rows * eighth)
            for q in range(4):
                block = block_of(q, 0)
                go_table(block, 0).wait_send()
                if q == 0 or (q == 1 and not end):
                    go_table(block, 1).wait_send()
                if q != 1 and not end:
                    go_table(block, 2).wait_send()
            if end:
                drain(12, 0, 2 * whole_rows * side)

        def items_of(q, h):
            if h < 0:
                return [(mine if h == -1 else other, g) for g in range(pieces)]
            return [(2 * planes[q], h), (2 * planes[q] + 1, h)]

        last_stage = max(i for i, item in enumerate(order) if item[0] == "C")
        for i, (op, q, *rest) in enumerate(order):
            if op == "P":
                on_p(q, *rest)
            elif op == "Y":
                on_y(block_of(q, rest[0]), rest[1])
            elif op == "F":
                if rest[0] == -1:
                    for item in weight_copies:
                        item.wait()
                else:
                    if rest[0] == -2:
                        ready_own()
                    else:
                        ready(planes[q], rest[0])
                lift(items_of(q, rest[0]))
            elif op == "N":
                lower(items_of(q, rest[0]))
            elif op == "A":
                stage_a(planes[q], rest[0], not end and q == 0, end and q == 1)
            elif op == "Ba":
                stage_ba(planes[q], rest[0])
            elif op == "Bb":
                stage_bb(planes[q], rest[0])
            elif op == "C":
                stage_c(planes[q], rest[0], q > 0)
            elif op == "S":
                settle(q, planes[1:] if end else planes[2:])
            if i == last_stage:
                drain_all()
        drain(11, 0, (nz - 2 if end else nz - 1) * pieces * rows * quarter)

    @pl.when(at_end)
    def _():
        drive(END, True)

    @pl.when(~at_end)
    def _():
        drive(MIDDLE, False)


def dense(tokens, norm_gain, expert_ids, route_weights, gate_weight, up_weight, down_weight):
    rows, width = tokens.shape
    n_ep = lax.axis_size("ep")
    nz = n_ep // 2
    pieces = len(XZ)
    ff = gate_weight.shape[2]
    quarter = width // lax.axis_size("tp")
    eighth = quarter // 2
    vmem = pl.BlockSpec(memory_space=pltpu.VMEM)
    hbm = pl.BlockSpec(memory_space=pl.ANY)
    bf16 = jnp.bfloat16
    dma = pltpu.SemaphoreType.DMA
    return pl.pallas_call(
        functools.partial(kernel, n_ep),
        out_shape=jax.ShapeDtypeStruct((rows, quarter), bf16),
        in_specs=[hbm, vmem, vmem, vmem, hbm, hbm, hbm],
        out_specs=vmem,
        scratch_shapes=[
            pltpu.VMEM((rows, width), bf16),
            pltpu.VMEM((n_ep, rows, width), bf16),
            pltpu.VMEM((n_ep, n_ep, rows), jnp.float32),
            pltpu.VMEM((rows, 128), jnp.float32),
            pltpu.VMEM((width, ff), bf16),
            pltpu.VMEM((width, ff), bf16),
            pltpu.VMEM((ff, width), bf16),
            pltpu.VMEM((rows, ff), bf16),
            pltpu.VMEM((n_ep, rows, width), bf16),
            pltpu.VMEM((n_ep, rows, 2 * quarter), bf16),
            pltpu.VMEM((n_ep, rows, eighth), bf16),
            pltpu.VMEM((nz, rows, eighth), bf16),
            pltpu.VMEM((nz, rows, 2 * eighth), bf16),
            pltpu.VMEM((nz, rows, eighth), bf16),
            pltpu.VMEM((nz, rows, quarter), bf16),
            pltpu.VMEM((nz, rows, quarter), bf16),
            pltpu.VMEM((2, rows, 2 * quarter), bf16),
            dma((pieces,)), dma((3,)), dma((13, nz)), dma((3, n_ep)), dma((n_ep,)),
            dma((n_ep, pieces)), dma((n_ep, pieces)), dma((nz, pieces)),
            dma((nz, pieces)), dma((nz, pieces)), dma((nz, pieces)),
            dma((nz, pieces)), dma((nz, pieces)), dma((pieces,)), dma((pieces,)),
        ],
        compiler_params=pltpu.CompilerParams(
            collective_id=0, has_side_effects=True, vmem_limit_bytes=60 * 1024 * 1024
        ),
    )(
        tokens, norm_gain[None, :], expert_ids.T, route_weights.T,
        gate_weight, up_weight, down_weight,
    )


def per_device(tokens, norm_gain, expert_ids, route_weights, gate_weight, up_weight, down_weight):
    tok_dev, top = expert_ids.shape
    experts = gate_weight.shape[0] * lax.axis_size("ep")
    whole = gate_weight.shape[0] == 1 and 2 * tok_dev * top // experts >= tok_dev
    whole = whole and lax.axis_size("tp") == 4 and lax.axis_size("ep") == 8
    form = dense if whole and tokens.shape[1] % 2048 == 0 else routed
    return form(
        tokens, norm_gain, expert_ids, route_weights, gate_weight, up_weight, down_weight
    )


def solution(mesh):
    in_specs = (
        P("ep", None),
        P(),
        P("ep", None),
        P("ep", None),
        P("ep", None, "tp"),
        P("ep", None, "tp"),
        P("ep", "tp", None),
    )
    return jax.shard_map(
        per_device, mesh=mesh, in_specs=in_specs, out_specs=P("ep", "tp"), check_vma=False
    )
```
